32 devices in a mesh: sp: 16 (over z, y, x), tp: 2 (over core).
Axes of the slice: x: 2, y: 2, z: 4, core: 2. Of those that a mesh axis runs over, the one named last changes fastest.
Arguments:
- stream: bfloat16 [2048, 2048], P(('sp', 'tp')), may hold values from -6 to 6
- wide_head_query: bfloat16 [2048, 1024], P('sp', 'tp'), may hold values from -6 to 6
- broad_attention_lookup_vectors: bfloat16 [2048, 1024], P('sp', 'tp'), may hold values from -6 to 6
- values_wide: bfloat16 [2048, 2048], P('sp', 'tp'), may hold values from -6 to 6
- query_narrow: bfloat16 [2048, 512], P('sp', 'tp'), may hold values from -6 to 6
- keys_narrow: bfloat16 [2048, 512], P('sp', 'tp'), may hold values from -6 to 6
- values_narrow: bfloat16 [2048, 1024], P('sp', 'tp'), may hold values from -6 to 6
- gate_wide: bfloat16 [2048, 2048], P('sp', 'tp'), may hold values from -6 to 6
- gate_narrow: bfloat16 [2048, 1024], P('sp', 'tp'), may hold values from -6 to 6
- log_decay: float32 [2, 8, 2048], P(None, 'tp', 'sp'), may hold values from -1.2 to 0, as said below
- gain_wide: bfloat16 [2048], P('tp'), may hold values from 0.099609375 to 1.8984375
- gain_narrow: bfloat16 [1024], P('tp'), may hold values from 0.099609375 to 1.8984375
- out_wide: bfloat16 [2048, 2048], P('tp'), may hold values from -0.109375 to 0.109375
- out_narrow: bfloat16 [1024, 2048], P('tp'), may hold values from -0.109375 to 0.109375
- gain_mix: bfloat16 [2048], replicated, may hold values from 0.099609375 to 1.8984375
- gain_pre: bfloat16 [2048], replicated, may hold values from 0.099609375 to 1.8984375
- gain_post: bfloat16 [2048], replicated, may hold values from 0.099609375 to 1.8984375
- weight_gate: bfloat16 [2048, 5120], P('sp', 'tp'), may hold values from -0.125 to 0.125
- weight_lin: bfloat16 [2048, 5120], P('sp', 'tp'), may hold values from -0.125 to 0.125
- weight_down: bfloat16 [2048, 5120], P('sp', 'tp'), may hold values from -0.078125 to 0.078125
- taps_gate: bfloat16 [3, 5120], P(None, 'tp'), may hold values from -3 to 3
- taps_lin: bfloat16 [3, 5120], P(None, 'tp'), may hold values from -3 to 3
Outputs:
- stream_out: bfloat16 [2048, 2048], P(('sp', 'tp'))
The draws below stay inside these ranges and needn't reach their ends.
Inputs may be any that keep to these rules, and one draw needn't show every extreme that they name: `log_decay`: the natural logarithm of the factor by which one head's retained state is multiplied at one position.
All inputs are finite; a program needn't handle non-finite values.
Results may differ from the reference program's by a relative error of at most 0.023.
Values may be sent and summed in bfloat16 or wider, within the bound.
A program may use at most 128 MiB of HBM per device.

```python
import math
import jax
import jax.numpy as jnp
from jax import lax

D = 2048
HEADS = 8
KW = 128
VW = 256
KN = 64
VN = 128
FF = 5120
CONV = 3
BLOCK = 128
TOKENS = 2048
N_TP = 2


def draw_log_decay(key, part):
    keys = jax.random.split(jax.random.fold_in(key, 11), 6)
    fast_share = 0.5
    fast = jax.random.uniform(keys[0], (2, HEADS, 1), jnp.float32) < fast_share
    fast_rate = jnp.exp(jax.random.uniform(keys[1], (2, HEADS, 1), jnp.float32, math.log(1.0 / 60.0), math.log(1.0 / 20.0)))
    slow_rate = jnp.exp(jax.random.uniform(keys[2], (2, HEADS, 1), jnp.float32, math.log(0.15), math.log(0.6))) / TOKENS
    forgetting_speed = jnp.where(fast, fast_rate, slow_rate)
    layer_groups_list = TOKENS // BLOCK
    multiplier_coefficient = jnp.exp(jax.random.uniform(keys[3], (2, HEADS, layer_groups_list), jnp.float32, math.log(0.5), math.log(2.0)))
    multiplier_coefficient = jnp.repeat(multiplier_coefficient, BLOCK, axis=2)
    spots = jax.random.randint(keys[4], (2, HEADS, 2), 0, TOKENS)
    layer_number_total = jnp.log(1.0 - jax.random.uniform(keys[5], (2, HEADS, 2), jnp.float32, 0.2, 0.4))
    agreeing_tally = spots[..., None] == jnp.arange(TOKENS, dtype=jnp.int32)[None, None, None, :]
    segment_span = jnp.sum(jnp.where(agreeing_tally, layer_number_total[..., None], 0.0), axis=2)
    return (-forgetting_speed * multiplier_coefficient + segment_span).astype(jnp.float32)


def steps_of(rng, extent, cuts, least, high):
    level, own = 1.0, jax.random.fold_in(rng, 6)
    for axis_at, parts in cuts:
        draws = jnp.exp(jax.random.uniform(jax.random.fold_in(own, axis_at), (parts,), jnp.float32, least / len(cuts), high / len(cuts)))
        level = level * jnp.repeat(draws, extent[axis_at] // parts).reshape([-1 if axis == axis_at else 1 for axis in range(len(extent))])
    return level


def bell_draw(stream_key, dims, deviation, bound, cuts=(), kind=jnp.bfloat16):
    values = jax.random.normal(stream_key, dims, jnp.float32) * deviation
    if len(cuts) > 0:
        values = steps_of(stream_key, dims, cuts, -0.22, 0.18) * values
    return jnp.clip(values, min=-bound, max=bound).astype(kind)


def setup_inputs(seed: int = 0) -> dict:
    seeds = jax.random.split(jax.random.key(seed), 23)
    stream = bell_draw(seeds[0], (TOKENS, D), 1.0, 6.0, ((0, 32),))
    wide_head_query = bell_draw(seeds[1], (TOKENS, HEADS * KW), 1.0, 6.0, ((0, 16), (1, 2)))
    broad_attention_lookup_vectors = bell_draw(seeds[2], (TOKENS, HEADS * KW), 1.0, 6.0, ((0, 16), (1, 2)))
    values_wide = bell_draw(seeds[3], (TOKENS, HEADS * VW), 1.0, 6.0, ((0, 16), (1, 2)))
    query_narrow = bell_draw(seeds[4], (TOKENS, HEADS * KN), 1.0, 6.0, ((0, 16), (1, 2)))
    keys_narrow = bell_draw(seeds[5], (TOKENS, HEADS * KN), 1.0, 6.0, ((0, 16), (1, 2)))
    values_narrow = bell_draw(seeds[6], (TOKENS, HEADS * VN), 1.0, 6.0, ((0, 16), (1, 2)))
    gate_wide = bell_draw(seeds[7], (TOKENS, HEADS * VW), 1.0, 6.0, ((0, 16), (1, 2)))
    gate_narrow = bell_draw(seeds[8], (TOKENS, HEADS * VN), 1.0, 6.0, ((0, 16), (1, 2)))
    log_decay = draw_log_decay(jax.random.fold_in(seeds[22], 71), 0)
    gain_wide = jnp.clip(1.0 + 0.18 * jax.random.normal(seeds[10], (HEADS * VW,), jnp.float32), 0.099609375, 1.8984375).astype(jnp.bfloat16)
    gain_narrow = jnp.clip(1.0 + 0.18 * jax.random.normal(seeds[11], (HEADS * VN,), jnp.float32), 0.099609375, 1.8984375).astype(jnp.bfloat16)
    out_wide = bell_draw(seeds[12], (HEADS * VW, D), (HEADS * (VW + VN)) ** -0.5, 0.109375, ((0, 2),))
    out_narrow = bell_draw(seeds[13], (HEADS * VN, D), (HEADS * (VW + VN)) ** -0.5, 0.109375, ((0, 2),))
    gain_mix = jnp.clip(1.0 + 0.18 * jax.random.normal(seeds[14], (D,), jnp.float32), 0.099609375, 1.8984375).astype(jnp.bfloat16)
    gain_pre = jnp.clip(1.0 + 0.18 * jax.random.normal(seeds[15], (D,), jnp.float32), 0.099609375, 1.8984375).astype(jnp.bfloat16)
    gain_post = jnp.clip(1.0 + 0.18 * jax.random.normal(seeds[16], (D,), jnp.float32), 0.099609375, 1.8984375).astype(jnp.bfloat16)
    weight_gate = bell_draw(seeds[17], (D, FF), D ** -0.5, 0.125, ((0, 16), (1, 2)))
    weight_lin = bell_draw(seeds[18], (D, FF), D ** -0.5, 0.125, ((0, 16), (1, 2)))
    weight_down = bell_draw(seeds[19], (D, FF), FF ** -0.5, 0.078125, ((0, 16), (1, 2)))
    taps_gate = bell_draw(seeds[20], (CONV, FF), 0.58, 3.0, ((1, 2),))
    taps_lin = bell_draw(seeds[21], (CONV, FF), 0.58, 3.0, ((1, 2),))
    return dict(stream=stream, wide_head_query=wide_head_query, broad_attention_lookup_vectors=broad_attention_lookup_vectors, values_wide=values_wide, query_narrow=query_narrow, keys_narrow=keys_narrow, values_narrow=values_narrow, gate_wide=gate_wide, gate_narrow=gate_narrow, log_decay=log_decay, gain_wide=gain_wide, gain_narrow=gain_narrow, out_wide=out_wide, out_narrow=out_narrow, gain_mix=gain_mix, gain_pre=gain_pre, gain_post=gain_post, weight_gate=weight_gate, weight_lin=weight_lin, weight_down=weight_down, taps_gate=taps_gate, taps_lin=taps_lin)


EPS = 1e-06
THETA = 10000.0

def rotate(block, positions):
    width = block.shape[-1]
    half = width // 2
    frequency = THETA ** (-(jnp.arange(half, dtype=jnp.float32) * 2.0 / width))
    angles = positions.astype(jnp.float32)[:, None] * frequency[None, :]
    cosine = jnp.cos(angles)[:, None, :]
    sine = jnp.sin(angles)[:, None, :]
    values = block.astype(jnp.float32)
    first = values[..., :half]
    second = values[..., half:]
    return jnp.concatenate([first * cosine - second * sine, second * cosine + first * sine], axis=-1)

def block_step(state, inputs):
    query, keys, values, log_rate = inputs
    running = jnp.cumsum(log_rate, axis=1)
    length = running.shape[1]
    index = jnp.arange(length)
    lower = (index[:, None] >= index[None, :])[None]
    spread = jnp.where(lower, jnp.exp(jnp.where(lower, running[:, :, None] - running[:, None, :], 0.0)), 0.0)
    query_f = query.astype(jnp.float32)
    values_f = values.astype(jnp.float32)
    scores = jnp.einsum('ihd,jhd->hij', query_f, keys.astype(jnp.float32), precision=lax.Precision.HIGHEST) * spread
    scores = lax.optimization_barrier(scores.astype(jnp.bfloat16)).astype(jnp.float32)
    inner = jnp.einsum('hij,jhe->ihe', scores, values_f, precision=lax.Precision.HIGHEST)
    lifted = query_f * jnp.exp(running).T[:, :, None]
    cross = jnp.einsum('ihd,hde->ihe', lifted, state, precision=lax.Precision.HIGHEST)
    tail = running[:, -1:]
    scaled = keys.astype(jnp.float32) * jnp.exp(tail - running).T[:, :, None]
    scaled = lax.optimization_barrier(scaled.astype(jnp.bfloat16)).astype(jnp.float32)
    update = jnp.einsum('jhd,jhe->hde', scaled, values_f, precision=lax.Precision.HIGHEST)
    state = state * jnp.exp(tail)[:, :, None] + update
    return (state, inner + cross)

def retain(query, keys, values, log_rate, head_dim, value_dim):
    total = query.shape[0]
    heads = query.shape[1] // head_dim
    positions = jnp.arange(total, dtype=jnp.int32)
    rotated_query = rotate(query.reshape(total, heads, head_dim), positions).astype(jnp.bfloat16)
    rotated_keys = (rotate(keys.reshape(total, heads, head_dim), positions) * head_dim ** (-0.5)).astype(jnp.bfloat16)
    layer_groups_list = total // BLOCK

    def split(array):
        return array.reshape(layer_groups_list, BLOCK, heads, array.shape[-1])
    rates = jnp.transpose(log_rate.reshape(heads, layer_groups_list, BLOCK), (1, 0, 2))
    start = jnp.zeros((heads, head_dim, value_dim), jnp.float32)
    inputs = (split(rotated_query), split(rotated_keys), split(values.reshape(total, heads, value_dim)), rates)
    _, outs = lax.scan(block_step, start, inputs)
    return outs.reshape(total, heads, value_dim)

def gate_heads(retained, gain, gate):
    mean = lax.optimization_barrier(jnp.mean(retained, axis=-1, keepdims=True))
    centred = retained - mean
    variance = lax.optimization_barrier(jnp.mean(centred * centred, axis=-1, keepdims=True))
    normed = (centred * lax.rsqrt(variance + EPS)).reshape(retained.shape[0], -1)
    return (normed * gain.astype(jnp.float32) * jax.nn.silu(gate.astype(jnp.float32))).astype(jnp.bfloat16)

def scale_rows(rows, gain):
    return rows * lax.rsqrt(lax.optimization_barrier(jnp.mean(rows * rows, axis=-1, keepdims=True)) + EPS) * gain.astype(jnp.float32)

def causal_taps(upward, taps):
    width = taps.shape[0]
    total = upward.shape[0]
    padded_rows = jnp.concatenate([jnp.zeros((width - 1, upward.shape[1]), upward.dtype), upward], axis=0).astype(jnp.float32)
    smooth = jnp.zeros((total, upward.shape[1]), jnp.float32)
    for tap_index in range(width):
        smooth = smooth + taps[tap_index].astype(jnp.float32)[None, :] * padded_rows[tap_index:tap_index + total]
    return smooth

def reference(stream, wide_head_query, broad_attention_lookup_vectors, values_wide, query_narrow, keys_narrow, values_narrow, gate_wide, gate_narrow, log_decay, gain_wide, gain_narrow, out_wide, out_narrow, gain_mix, gain_pre, gain_post, weight_gate, weight_lin, weight_down, taps_gate, taps_lin):
    wide = gate_heads(retain(wide_head_query, broad_attention_lookup_vectors, values_wide, log_decay[0], KW, VW), gain_wide, gate_wide)
    narrow = gate_heads(retain(query_narrow, keys_narrow, values_narrow, log_decay[1], KN, VN), gain_narrow, gate_narrow)
    share = HEADS // N_TP
    mixed = jnp.zeros((TOKENS, D), jnp.float32)
    for group in range(N_TP):
        lo_wide, hi_wide = (group * share * VW, (group + 1) * share * VW)
        lo_narrow, hi_narrow = (group * share * VN, (group + 1) * share * VN)
        partial_sum = jnp.dot(wide[:, lo_wide:hi_wide], out_wide[lo_wide:hi_wide], preferred_element_type=jnp.float32)
        partial_sum = partial_sum + jnp.dot(narrow[:, lo_narrow:hi_narrow], out_narrow[lo_narrow:hi_narrow], preferred_element_type=jnp.float32)
        mixed = mixed + lax.optimization_barrier(partial_sum.astype(jnp.bfloat16)).astype(jnp.float32)
    resid = lax.optimization_barrier((stream.astype(jnp.float32) + scale_rows(mixed, gain_mix)).astype(jnp.bfloat16))
    normed_in = scale_rows(resid.astype(jnp.float32), gain_pre).astype(jnp.bfloat16)
    up_gate = jnp.dot(normed_in, weight_gate, preferred_element_type=jnp.float32).astype(jnp.bfloat16)
    up_lin = jnp.dot(normed_in, weight_lin, preferred_element_type=jnp.float32).astype(jnp.bfloat16)
    smooth_gate = causal_taps(up_gate, taps_gate)
    smooth_lin = causal_taps(up_lin, taps_lin)
    hidden = (jax.nn.silu(smooth_gate) * smooth_lin).astype(jnp.bfloat16)
    units = FF // N_TP
    fed = jnp.zeros((TOKENS, D), jnp.float32)
    for group in range(N_TP):
        partial_sum = lax.dot_general(hidden[:, group * units:(group + 1) * units], weight_down[:, group * units:(group + 1) * units], (((1,), (1,)), ((), ())), preferred_element_type=jnp.float32)
        fed = fed + lax.optimization_barrier(partial_sum.astype(jnp.bfloat16)).astype(jnp.float32)
    return (resid.astype(jnp.float32) + scale_rows(fed, gain_post)).astype(jnp.bfloat16)
```

```python
import jax
import jax.numpy as jnp
from jax import lax
from jax.sharding import PartitionSpec as P

KW = 128
VW = 256
KN = 64
VN = 128
BLOCK = 128


EPS = 1e-06
THETA = 10000.0


def passed_along(value, axis, steps):
    count = lax.axis_size(axis)
    first, last = (max(0, -steps), min(count, count - steps))
    return lax.ppermute(value, axis, [(source, source + steps) for source in range(first, last)])


def rotate(block, positions):
    width = block.shape[-1]
    half = width // 2
    frequency = THETA ** (-(jnp.arange(half, dtype=jnp.float32) * 2.0 / width))
    angles = positions.astype(jnp.float32)[:, None] * frequency[None, :]
    cosine = jnp.cos(angles)[:, None, :]
    sine = jnp.sin(angles)[:, None, :]
    values = block.astype(jnp.float32)
    first = values[..., :half]
    second = values[..., half:]
    return jnp.concatenate(
        [first * cosine - second * sine, second * cosine + first * sine], axis=-1
    )


def block_step(state, inputs):
    query, keys, values, log_rate = inputs
    running = jnp.cumsum(log_rate, axis=1)
    length = running.shape[1]
    index = jnp.arange(length)
    lower = (index[:, None] >= index[None, :])[None]
    spread = jnp.where(
        lower, jnp.exp(jnp.where(lower, running[:, :, None] - running[:, None, :], 0.0)), 0.0
    )
    scores = (
        jnp.einsum("ihd,jhd->hij", query, keys, preferred_element_type=jnp.float32) * spread
    ).astype(jnp.bfloat16)
    inner = jnp.einsum("hij,jhe->ihe", scores, values, preferred_element_type=jnp.float32)
    lifted = query.astype(jnp.float32) * jnp.exp(running).T[:, :, None]
    cross = jnp.einsum("ihd,hde->ihe", lifted, state, precision=lax.Precision.HIGHEST)
    tail = running[:, -1:]
    scaled = (keys.astype(jnp.float32) * jnp.exp(tail - running).T[:, :, None]).astype(jnp.bfloat16)
    update = jnp.einsum("jhd,jhe->hde", scaled, values, preferred_element_type=jnp.float32)
    state = state * jnp.exp(tail)[:, :, None] + update
    return (state, inner + cross)


def kept_nearby_memory(query, keys, values, log_rate, head_dim, value_dim, offset):
    rows = query.shape[0]
    heads = query.shape[1] // head_dim
    positions = offset + jnp.arange(rows, dtype=jnp.int32)
    rotated_query = rotate(query.reshape(rows, heads, head_dim), positions).astype(jnp.bfloat16)
    rotated_keys = (
        rotate(keys.reshape(rows, heads, head_dim), positions) * head_dim ** (-0.5)
    ).astype(jnp.bfloat16)
    layer_groups_list = rows // BLOCK

    def split(array):
        return array.reshape(layer_groups_list, BLOCK, heads, array.shape[-1])

    rates = jnp.transpose(log_rate.reshape(heads, layer_groups_list, BLOCK), (1, 0, 2))
    start = jnp.zeros((heads, head_dim, value_dim), jnp.float32)
    inputs = (
        split(rotated_query),
        split(rotated_keys),
        split(values.reshape(rows, heads, value_dim)),
        rates,
    )
    state, outs = lax.scan(block_step, start, inputs)
    return (rotated_query, outs.reshape(rows, heads, value_dim), state)


def carried(rotated_query, log_rate, state_in):
    lifted = rotated_query.astype(jnp.float32) * jnp.exp(jnp.cumsum(log_rate, axis=1)).T[:, :, None]
    return jnp.einsum("ihd,hde->ihe", lifted, state_in, precision=lax.Precision.HIGHEST)


def gate_heads(retained, gain, gate):
    mean = jnp.mean(retained, axis=-1, keepdims=True)
    centred = retained - mean
    variance = jnp.mean(centred * centred, axis=-1, keepdims=True)
    normed = (centred * lax.rsqrt(variance + EPS)).reshape(retained.shape[0], -1)
    return (normed * gain.astype(jnp.float32) * jax.nn.silu(gate.astype(jnp.float32))).astype(
        jnp.bfloat16
    )


def scale_rows(rows, gain):
    return (
        rows
        * lax.rsqrt(jnp.mean(rows * rows, axis=-1, keepdims=True) + EPS)
        * gain.astype(jnp.float32)
    )


def causal_taps(upward, before, taps):
    width = taps.shape[0]
    total = upward.shape[0]
    padded_rows = jnp.concatenate([before, upward], axis=0).astype(jnp.float32)
    smooth = jnp.zeros((total, upward.shape[1]), jnp.float32)
    for tap_index in range(width):
        smooth = (
            smooth
            + taps[tap_index].astype(jnp.float32)[None, :]
            * padded_rows[tap_index : tap_index + total]
        )
    return smooth


def swap_blocks(blocks, axis):
    return lax.all_to_all(blocks, axis, 0, 0, tiled=False)


def share_rows(parts, axis):
    count = lax.axis_size(axis)
    place = lax.axis_index(axis)
    total = lax.dynamic_index_in_dim(parts, place, 0, False).astype(jnp.float32)
    for step in range(1, count):
        piece = lax.dynamic_index_in_dim(parts, (place + step) % count, 0, False)
        moved = lax.ppermute(piece, axis, [(i, (i + step) % count) for i in range(count)])
        total = total + moved.astype(jnp.float32)
    return total


def carried_in(states, decays, axis):
    count = lax.axis_size(axis)
    place = lax.axis_index(axis)
    lanes = states[-1].shape[-1]
    flat = jnp.concatenate([s.reshape(-1, lanes) for s in states]).astype(jnp.bfloat16)
    rates = jnp.concatenate(
        [jnp.repeat(d, s.size // s.shape[0] // lanes) for s, d in zip(states, decays)]
    )
    share = flat.shape[0] // count
    every = lax.all_gather(rates, axis)
    mine = lax.dynamic_slice_in_dim(every, place * share, share, 1)
    got = swap_blocks(flat.reshape(count, share, lanes), axis).astype(jnp.float32)
    level = jnp.zeros((share, lanes), jnp.float32)
    before = []
    for step in range(count):
        before.append(level.astype(jnp.bfloat16))
        level = level * mine[step][:, None] + got[step]
    back = swap_blocks(jnp.stack(before), axis).reshape(-1, lanes).astype(jnp.float32)
    outs, at = [], 0
    for s in states:
        rows = s.size // lanes
        outs.append(back[at : at + rows].reshape(s.shape))
        at += rows
    return outs


def feed_by_weights(normed_in, weight_gate, weight_lin, weight_down, taps_gate, taps_lin):
    normed_all = lax.all_gather(normed_in, "tp", axis=0, tiled=True)
    rows = normed_all.shape[0]
    whole_gate, whole_lin = (
        lax.all_gather(weight_gate, "sp", axis=0, tiled=True),
        lax.all_gather(weight_lin, "sp", axis=0, tiled=True),
    )
    up_gate = jnp.dot(normed_all, whole_gate, preferred_element_type=jnp.float32).astype(
        jnp.bfloat16
    )
    up_lin = jnp.dot(normed_all, whole_lin, preferred_element_type=jnp.float32).astype(jnp.bfloat16)
    reach = taps_gate.shape[0] - 1
    before_gate, before_lin = passed_along(
        (up_gate[rows - reach :], up_lin[rows - reach :]), "sp", 1
    )
    smooth_gate = causal_taps(up_gate, before_gate, taps_gate)
    smooth_lin = causal_taps(up_lin, before_lin, taps_lin)
    hidden = (jax.nn.silu(smooth_gate) * smooth_lin).astype(jnp.bfloat16)
    terms = lax.dot_general(
        hidden,
        lax.all_gather(weight_down, "sp", axis=0, tiled=True),
        (((1,), (1,)), ((), ())),
        preferred_element_type=jnp.float32,
    )
    return lax.psum_scatter(
        terms.astype(jnp.bfloat16), "tp", scatter_dimension=0, tiled=True
    ).astype(jnp.float32)


def from_all(value, axis, dim):
    count = lax.axis_size(axis)
    found = [value]
    for step in range(1, count):
        found.append(lax.ppermute(value, axis, [(i, (i + step) % count) for i in range(count)]))
    return jnp.concatenate(found, axis=dim)


def unit_slices(weight_gate, weight_lin, weight_down, taps_gate, taps_lin):
    count = lax.axis_size("sp")
    place = lax.axis_index("sp")
    deep, units = weight_gate.shape
    share = units // count
    turned = jnp.stack([weight_gate.T, weight_lin.T, weight_down.T])
    blocks = turned.reshape(3, count, share, deep).transpose(1, 0, 2, 3)
    got = swap_blocks(blocks, "sp")
    mine = got.transpose(1, 2, 0, 3).reshape(3, share, count * deep)
    taps = jnp.stack([taps_gate, taps_lin])
    taps = lax.dynamic_slice_in_dim(taps, place * share, share, 2)
    return from_all(mine, "tp", 1), from_all(taps, "tp", 2)


def feed_by_tokens(normed_in, weights, taps):
    count = lax.axis_size("sp")
    n_tp = lax.axis_size("tp")
    rows, width = normed_in.shape
    tokens = lax.all_gather(normed_in, "sp", axis=0, tiled=True)
    flat = weights[:2].reshape(-1, width)
    ups = lax.dot_general(
        tokens, flat, (((1,), (1,)), ((), ())), preferred_element_type=jnp.float32
    ).astype(jnp.bfloat16)
    units = flat.shape[0] // 2
    ups = ups.reshape(count, rows, 2 * units)
    reach = taps.shape[1] - 1
    tails = ups[:, rows - reach :]
    prior = lax.ppermute(tails, "tp", [(i, (i + 1) % n_tp) for i in range(n_tp)])
    prior = jnp.roll(prior.reshape(count, reach, 2, n_tp, -1), 1, axis=3).reshape(prior.shape)
    shifted = jnp.concatenate([jnp.zeros_like(prior[:1]), prior[:-1]], axis=0)
    prior = jnp.where(lax.axis_index("tp") == 0, shifted, prior)
    padded = jnp.concatenate([prior, ups], axis=1).astype(jnp.float32)
    taps = jnp.concatenate([taps[0], taps[1]], axis=1).astype(jnp.float32)
    smooth = sum(taps[j] * padded[:, j : j + rows] for j in range(reach + 1))
    hidden = (jax.nn.silu(smooth[..., :units]) * smooth[..., units:]).astype(jnp.bfloat16)
    terms = jnp.dot(
        hidden.reshape(count * rows, units), weights[2], preferred_element_type=jnp.float32
    )
    return lax.psum_scatter(
        terms.astype(jnp.bfloat16), "sp", scatter_dimension=0, tiled=True
    ).astype(jnp.float32)


def body(
    stream,
    wide_head_query,
    broad_attention_lookup_vectors,
    values_wide,
    query_narrow,
    keys_narrow,
    values_narrow,
    gate_wide,
    gate_narrow,
    log_decay,
    gain_wide,
    gain_narrow,
    out_wide,
    out_narrow,
    gain_mix,
    gain_pre,
    gain_post,
    weight_gate,
    weight_lin,
    weight_down,
    taps_gate,
    taps_lin,
):
    rows = wide_head_query.shape[0]
    count = lax.axis_size("sp")
    n_tp = lax.axis_size("tp")
    width = stream.shape[1]
    units = weight_gate.shape[1]
    by_tokens = 2 * count * rows < 3 * units and units % (count * 16) == 0
    if by_tokens:
        weights, taps = unit_slices(weight_gate, weight_lin, weight_down, taps_gate, taps_lin)
    offset = lax.axis_index("sp") * rows
    rates_wide = log_decay[0]
    rates_narrow = log_decay[1]
    rot_wide, local_wide, state_wide = kept_nearby_memory(
        wide_head_query, broad_attention_lookup_vectors, values_wide, rates_wide, KW, VW, offset
    )
    rot_narrow, local_narrow, state_narrow = kept_nearby_memory(
        query_narrow, keys_narrow, values_narrow, rates_narrow, KN, VN, offset
    )
    incoming = carried_in(
        (state_wide, state_narrow),
        (jnp.exp(jnp.sum(rates_wide, axis=1)), jnp.exp(jnp.sum(rates_narrow, axis=1))),
        "sp",
    )
    gated_wide = gate_heads(
        local_wide + carried(rot_wide, rates_wide, incoming[0]), gain_wide, gate_wide
    )
    gated_narrow = gate_heads(
        local_narrow + carried(rot_narrow, rates_narrow, incoming[1]), gain_narrow, gate_narrow
    )
    part_wide = jnp.dot(gated_wide, out_wide, preferred_element_type=jnp.float32)
    part_narrow = jnp.dot(gated_narrow, out_narrow, preferred_element_type=jnp.float32)
    mixed = share_rows(
        (part_wide + part_narrow).astype(jnp.bfloat16).reshape(n_tp, rows // n_tp, width), "tp"
    )
    resid = (stream.astype(jnp.float32) + scale_rows(mixed, gain_mix)).astype(jnp.bfloat16)
    normed_in = scale_rows(resid.astype(jnp.float32), gain_pre).astype(jnp.bfloat16)
    if by_tokens:
        fed = feed_by_tokens(normed_in, weights, taps)
    else:
        fed = feed_by_weights(normed_in, weight_gate, weight_lin, weight_down, taps_gate, taps_lin)
    return (resid.astype(jnp.float32) + scale_rows(fed, gain_post)).astype(jnp.bfloat16)


def solution(mesh):
    in_specs = (
        P(("sp", "tp"), None),
        P("sp", "tp"),
        P("sp", "tp"),
        P("sp", "tp"),
        P("sp", "tp"),
        P("sp", "tp"),
        P("sp", "tp"),
        P("sp", "tp"),
        P("sp", "tp"),
        P(None, "tp", "sp"),
        P("tp"),
        P("tp"),
        P("tp", None),
        P("tp", None),
        P(),
        P(),
        P(),
        P("sp", "tp"),
        P("sp", "tp"),
        P("sp", "tp"),
        P(None, "tp"),
        P(None, "tp"),
    )
    out_specs = P(("sp", "tp"), None)
    return jax.shard_map(body, mesh=mesh, in_specs=in_specs, out_specs=out_specs, check_vma=False)
```

```python
import jax
import jax.numpy as jnp
from jax import lax
from jax.sharding import PartitionSpec as P

KW = 128
VW = 256
KN = 64
VN = 128
BLOCK = 128


EPS = 1e-06
THETA = 10000.0


def passed_along(value, axis, steps):
    count = lax.axis_size(axis)
    first, last = (max(0, -steps), min(count, count - steps))
    return lax.ppermute(value, axis, [(source, source + steps) for source in range(first, last)])


def rotate(block, positions):
    width = block.shape[-1]
    half = width // 2
    frequency = THETA ** (-(jnp.arange(half, dtype=jnp.float32) * 2.0 / width))
    angles = positions.astype(jnp.float32)[:, None] * frequency[None, :]
    cosine = jnp.cos(angles)[:, None, :]
    sine = jnp.sin(angles)[:, None, :]
    values = block.astype(jnp.float32)
    first = values[..., :half]
    second = values[..., half:]
    return jnp.concatenate(
        [first * cosine - second * sine, second * cosine + first * sine], axis=-1
    )


def block_step(state, inputs):
    query, keys, values, log_rate = inputs
    running = jnp.cumsum(log_rate, axis=1)
    length = running.shape[1]
    index = jnp.arange(length)
    lower = (index[:, None] >= index[None, :])[None]
    spread = jnp.where(
        lower, jnp.exp(jnp.where(lower, running[:, :, None] - running[:, None, :], 0.0)), 0.0
    )
    scores = (
        jnp.einsum("ihd,jhd->hij", query, keys, preferred_element_type=jnp.float32) * spread
    ).astype(jnp.bfloat16)
    inner = jnp.einsum("hij,jhe->ihe", scores, values, preferred_element_type=jnp.float32)
    lifted = query.astype(jnp.float32) * jnp.exp(running).T[:, :, None]
    cross = jnp.einsum("ihd,hde->ihe", lifted, state, precision=lax.Precision.HIGHEST)
    tail = running[:, -1:]
    scaled = (keys.astype(jnp.float32) * jnp.exp(tail - running).T[:, :, None]).astype(jnp.bfloat16)
    update = jnp.einsum("jhd,jhe->hde", scaled, values, preferred_element_type=jnp.float32)
    state = state * jnp.exp(tail)[:, :, None] + update
    return (state, inner + cross)


def kept_nearby_memory(query, keys, values, log_rate, head_dim, value_dim, offset):
    rows = query.shape[0]
    heads = query.shape[1] // head_dim
    positions = offset + jnp.arange(rows, dtype=jnp.int32)
    rotated_query = rotate(query.reshape(rows, heads, head_dim), positions).astype(jnp.bfloat16)
    rotated_keys = (
        rotate(keys.reshape(rows, heads, head_dim), positions) * head_dim ** (-0.5)
    ).astype(jnp.bfloat16)
    layer_groups_list = rows // BLOCK

    def split(array):
        return array.reshape(layer_groups_list, BLOCK, heads, array.shape[-1])

    rates = jnp.transpose(log_rate.reshape(heads, layer_groups_list, BLOCK), (1, 0, 2))
    start = jnp.zeros((heads, head_dim, value_dim), jnp.float32)
    inputs = (
        split(rotated_query),
        split(rotated_keys),
        split(values.reshape(rows, heads, value_dim)),
        rates,
    )
    state, outs = lax.scan(block_step, start, inputs)
    return (rotated_query, outs.reshape(rows, heads, value_dim), state)


def carried(rotated_query, log_rate, state_in):
    lifted = rotated_query.astype(jnp.float32) * jnp.exp(jnp.cumsum(log_rate, axis=1)).T[:, :, None]
    return jnp.einsum("ihd,hde->ihe", lifted, state_in, precision=lax.Precision.HIGHEST)


def gate_heads(retained, gain, gate):
    mean = jnp.mean(retained, axis=-1, keepdims=True)
    centred = retained - mean
    variance = jnp.mean(centred * centred, axis=-1, keepdims=True)
    normed = (centred * lax.rsqrt(variance + EPS)).reshape(retained.shape[0], -1)
    return (normed * gain.astype(jnp.float32) * jax.nn.silu(gate.astype(jnp.float32))).astype(
        jnp.bfloat16
    )


def scale_rows(rows, gain):
    return (
        rows
        * lax.rsqrt(jnp.mean(rows * rows, axis=-1, keepdims=True) + EPS)
        * gain.astype(jnp.float32)
    )


def causal_taps(upward, before, taps):
    width = taps.shape[0]
    total = upward.shape[0]
    padded_rows = jnp.concatenate([before, upward], axis=0).astype(jnp.float32)
    smooth = jnp.zeros((total, upward.shape[1]), jnp.float32)
    for tap_index in range(width):
        smooth = (
            smooth
            + taps[tap_index].astype(jnp.float32)[None, :]
            * padded_rows[tap_index : tap_index + total]
        )
    return smooth


def swap_blocks(blocks, axis):
    return lax.all_to_all(blocks, axis, 0, 0, tiled=False)


def share_rows(parts, axis):
    count = lax.axis_size(axis)
    place = lax.axis_index(axis)
    total = lax.dynamic_index_in_dim(parts, place, 0, False).astype(jnp.float32)
    for step in range(1, count):
        piece = lax.dynamic_index_in_dim(parts, (place + step) % count, 0, False)
        moved = lax.ppermute(piece, axis, [(i, (i + step) % count) for i in range(count)])
        total = total + moved.astype(jnp.float32)
    return total


def carried_in(states, totals, axis):
    count = lax.axis_size(axis)
    lanes = states[-1].shape[-1]
    flat = jnp.concatenate([s.reshape(-1, lanes) for s in states]).astype(jnp.bfloat16)
    rates = jnp.concatenate(
        [jnp.repeat(d, s.size // s.shape[0] // lanes) for s, d in zip(states, totals)]
    )
    share = flat.shape[0] // count
    rates = rates.reshape(count, share)
    rates = jnp.pad(rates, ((0, 0), (0, -share % lanes)))
    parts, left = [], rates
    for _ in range(3):
        parts.append(left.astype(jnp.bfloat16))
        left = left - parts[-1].astype(jnp.float32)
    parts = [part.reshape(count, -1, lanes) for part in parts]
    sent = jnp.concatenate([flat.reshape(count, share, lanes)] + parts, axis=1)
    got = swap_blocks(sent, axis).astype(jnp.float32)
    parts = jnp.split(got[:, share:], 3, axis=1)
    logs = (parts[0] + parts[1] + parts[2]).reshape(count, -1)[:, :share]
    own = got[:, :share]
    steps = jnp.arange(count)
    between = (steps[None, None] > steps[None, :, None]) & (
        steps[None, None] < steps[:, None, None]
    )
    span = jnp.sum(jnp.where(between[..., None], logs[None, None], 0.0), axis=2)
    factor = jnp.where((steps[None] < steps[:, None])[..., None], jnp.exp(span), 0.0)
    before = sum(factor[:, step, :, None] * own[step][None] for step in range(count))
    back = swap_blocks(before.astype(jnp.bfloat16), axis).reshape(-1, lanes).astype(jnp.float32)
    outs, at = [], 0
    for s in states:
        rows = s.size // lanes
        outs.append(back[at : at + rows].reshape(s.shape))
        at += rows
    return outs


def feed_by_weights(normed_in, weight_gate, weight_lin, weight_down, taps_gate, taps_lin):
    normed_all = lax.all_gather(normed_in, "tp", axis=0, tiled=True)
    rows = normed_all.shape[0]
    whole_gate, whole_lin = (
        lax.all_gather(weight_gate, "sp", axis=0, tiled=True),
        lax.all_gather(weight_lin, "sp", axis=0, tiled=True),
    )
    up_gate = jnp.dot(normed_all, whole_gate, preferred_element_type=jnp.float32).astype(
        jnp.bfloat16
    )
    up_lin = jnp.dot(normed_all, whole_lin, preferred_element_type=jnp.float32).astype(jnp.bfloat16)
    reach = taps_gate.shape[0] - 1
    before_gate, before_lin = passed_along(
        (up_gate[rows - reach :], up_lin[rows - reach :]), "sp", 1
    )
    smooth_gate = causal_taps(up_gate, before_gate, taps_gate)
    smooth_lin = causal_taps(up_lin, before_lin, taps_lin)
    hidden = (jax.nn.silu(smooth_gate) * smooth_lin).astype(jnp.bfloat16)
    terms = lax.dot_general(
        hidden,
        lax.all_gather(weight_down, "sp", axis=0, tiled=True),
        (((1,), (1,)), ((), ())),
        preferred_element_type=jnp.float32,
    )
    return lax.psum_scatter(
        terms.astype(jnp.bfloat16), "tp", scatter_dimension=0, tiled=True
    ).astype(jnp.float32)


def from_all(value, axis, dim):
    count = lax.axis_size(axis)
    found = [value]
    for step in range(1, count):
        found.append(lax.ppermute(value, axis, [(i, (i + step) % count) for i in range(count)]))
    return jnp.concatenate(found, axis=dim)


def unit_slices(weight_gate, weight_lin, weight_down, taps_gate, taps_lin):
    count = lax.axis_size("sp")
    place = lax.axis_index("sp")
    deep, units = weight_gate.shape
    share = units // count
    turned = jnp.stack([weight_gate.T, weight_lin.T, weight_down.T])
    blocks = turned.reshape(3, count, share, deep).transpose(1, 0, 2, 3)
    got = swap_blocks(blocks, "sp")
    mine = got.transpose(1, 2, 0, 3).reshape(3, share, count * deep)
    taps = jnp.stack([taps_gate, taps_lin])
    taps = lax.dynamic_slice_in_dim(taps, place * share, share, 2)
    return from_all(mine, "tp", 1), from_all(taps, "tp", 2)


def flip(value, axis, bit):
    return lax.ppermute(
        value, axis, [(i, i ^ (1 << bit)) for i in range(lax.axis_size(axis))]
    )


def bits_of(count, swapped):
    bits = list(range(count.bit_length() - 1))
    if swapped:
        bits[:2] = bits[:2][::-1]
    return bits


def gather_around(value, axis, swapped):
    bits = bits_of(lax.axis_size(axis), swapped)
    for bit in bits[::-1]:
        value = jnp.stack([value, flip(value, axis, bit)])
    order = [bits.index(bit) for bit in sorted(bits, reverse=True)]
    value = value.transpose(*order, *range(len(bits), value.ndim))
    return value.reshape(-1, *value.shape[len(bits) :])


def add_around(value, axis, swapped):
    bits = bits_of(lax.axis_size(axis), swapped)
    value = value.reshape(*[2] * len(bits), *value.shape[1:])
    dims = sorted(bits, reverse=True)
    for bit in bits:
        at = dims.index(bit)
        dims.remove(bit)
        kept = lax.index_in_dim(value, 0, at, False).astype(jnp.float32)
        sent = lax.index_in_dim(value, 1, at, False).astype(jnp.bfloat16)
        value = kept + flip(sent, axis, bit).astype(jnp.float32)
        if dims:
            value = value.astype(jnp.bfloat16)
    return value


def feed_by_tokens(normed_in, weights, taps):
    count = lax.axis_size("sp")
    n_tp = lax.axis_size("tp")
    rows, width = normed_in.shape
    place = lax.axis_index("sp")
    half = width // 2
    flat = weights[:2].reshape(-1, width)
    units = flat.shape[0] // 2
    ups = 0.0
    for part in range(2):
        cut = slice(part * half, (part + 1) * half)
        tokens = gather_around(normed_in[:, cut], "sp", part == 1)
        ups = ups + lax.dot_general(
            tokens.reshape(count * rows, half),
            flat[:, cut],
            (((1,), (1,)), ((), ())),
            preferred_element_type=jnp.float32,
        )
    ups = ups.astype(jnp.bfloat16).reshape(count, rows, 2 * units)
    reach = taps.shape[1] - 1
    tails = ups[:, rows - reach :]
    prior = lax.ppermute(tails, "tp", [(i, (i + 1) % n_tp) for i in range(n_tp)])
    prior = jnp.roll(prior.reshape(count, reach, 2, n_tp, -1), 1, axis=3).reshape(prior.shape)
    blocks = place ^ jnp.arange(count)
    follows = (blocks[:, None] == blocks[None, :] + 1).astype(jnp.bfloat16)
    shifted = jnp.dot(
        follows, prior.reshape(count, -1), preferred_element_type=jnp.float32
    ).astype(jnp.bfloat16).reshape(prior.shape)
    prior = jnp.where(lax.axis_index("tp") == 0, shifted, prior)
    padded = jnp.concatenate([prior, ups], axis=1).astype(jnp.float32)
    taps = jnp.concatenate([taps[0], taps[1]], axis=1).astype(jnp.float32)
    smooth = sum(taps[j] * padded[:, j : j + rows] for j in range(reach + 1))
    hidden = (jax.nn.silu(smooth[..., :units]) * smooth[..., units:]).astype(jnp.bfloat16)
    hidden = hidden.reshape(count * rows, units)
    sums = []
    for part in range(2):
        cut = slice(part * half, (part + 1) * half)
        terms = jnp.dot(hidden, weights[2][:, cut], preferred_element_type=jnp.float32)
        terms = terms.astype(jnp.bfloat16).reshape(count, rows, half)
        sums.append(add_around(terms, "sp", part == 1))
    return jnp.concatenate(sums, axis=1)


def body(
    stream,
    wide_head_query,
    broad_attention_lookup_vectors,
    values_wide,
    query_narrow,
    keys_narrow,
    values_narrow,
    gate_wide,
    gate_narrow,
    log_decay,
    gain_wide,
    gain_narrow,
    out_wide,
    out_narrow,
    gain_mix,
    gain_pre,
    gain_post,
    weight_gate,
    weight_lin,
    weight_down,
    taps_gate,
    taps_lin,
):
    rows = wide_head_query.shape[0]
    count = lax.axis_size("sp")
    n_tp = lax.axis_size("tp")
    width = stream.shape[1]
    units = weight_gate.shape[1]
    by_tokens = 2 * count * rows < 3 * units and units % (count * 16) == 0
    by_tokens = by_tokens and count & (count - 1) == 0
    if by_tokens:
        weights, taps = unit_slices(weight_gate, weight_lin, weight_down, taps_gate, taps_lin)
    offset = lax.axis_index("sp") * rows
    rates_wide = log_decay[0]
    rates_narrow = log_decay[1]
    rot_wide, local_wide, state_wide = kept_nearby_memory(
        wide_head_query, broad_attention_lookup_vectors, values_wide, rates_wide, KW, VW, offset
    )
    rot_narrow, local_narrow, state_narrow = kept_nearby_memory(
        query_narrow, keys_narrow, values_narrow, rates_narrow, KN, VN, offset
    )
    incoming = carried_in(
        (state_wide, state_narrow),
        (jnp.sum(rates_wide, axis=1), jnp.sum(rates_narrow, axis=1)),
        "sp",
    )
    gated_wide = gate_heads(
        local_wide + carried(rot_wide, rates_wide, incoming[0]), gain_wide, gate_wide
    )
    gated_narrow = gate_heads(
        local_narrow + carried(rot_narrow, rates_narrow, incoming[1]), gain_narrow, gate_narrow
    )
    part_wide = jnp.dot(gated_wide, out_wide, preferred_element_type=jnp.float32)
    part_narrow = jnp.dot(gated_narrow, out_narrow, preferred_element_type=jnp.float32)
    mixed = share_rows(
        (part_wide + part_narrow).astype(jnp.bfloat16).reshape(n_tp, rows // n_tp, width), "tp"
    )
    resid = (stream.astype(jnp.float32) + scale_rows(mixed, gain_mix)).astype(jnp.bfloat16)
    normed_in = scale_rows(resid.astype(jnp.float32), gain_pre).astype(jnp.bfloat16)
    if by_tokens:
        fed = feed_by_tokens(normed_in, weights, taps)
    else:
        fed = feed_by_weights(normed_in, weight_gate, weight_lin, weight_down, taps_gate, taps_lin)
    return (resid.astype(jnp.float32) + scale_rows(fed, gain_post)).astype(jnp.bfloat16)


def solution(mesh):
    in_specs = (
        P(("sp", "tp"), None),
        P("sp", "tp"),
        P("sp", "tp"),
        P("sp", "tp"),
        P("sp", "tp"),
        P("sp", "tp"),
        P("sp", "tp"),
        P("sp", "tp"),
        P("sp", "tp"),
        P(None, "tp", "sp"),
        P("tp"),
        P("tp"),
        P("tp", None),
        P("tp", None),
        P(),
        P(),
        P(),
        P("sp", "tp"),
        P("sp", "tp"),
        P("sp", "tp"),
        P(None, "tp"),
        P(None, "tp"),
    )
    out_specs = P(("sp", "tp"), None)
    return jax.shard_map(body, mesh=mesh, in_specs=in_specs, out_specs=out_specs, check_vma=False)
```
